32 devices in a mesh: sp: 8 (over z, y), tp: 4 (over x, core).
Axes of the slice: x: 2, y: 2, z: 4, core: 2. Of those that a mesh axis runs over, the one named last changes fastest.
Arguments:
- stream: bfloat16 [1536, 2048], P('sp'), may hold values from -6 to 6
- upstream: bfloat16 [1536, 2048], P('sp'), may hold values from -6 to 6
- expert_gain: float32 [2048], replicated, may hold values from 0.1 to 1.9
- expert_ids: int32 [1536, 2], P('sp'), may hold values from 0 to 7, all different within a row; in each aligned block of 192 rows (0 to 191, 192 to 383, ...) at most 60 rows name the same one
- group_weight: float32 [1536], P('sp'), may hold values from 0.25 to 1
- pair_scores: float32 [1536, 2], P('sp'), may hold values from -6 to 6
- gate_weight: bfloat16 [8, 2048, 1024], P('sp', None, 'tp'), may hold values from -0.125 to 0.125
- up_weight: bfloat16 [8, 2048, 1024], P('sp', None, 'tp'), may hold values from -0.125 to 0.125
- down_weight: bfloat16 [8, 1024, 2048], P('sp', 'tp'), may hold values from -0.1875 to 0.1875
- mixer_weight: bfloat16 [1024, 2048], P('tp'), may hold values from -0.1875 to 0.1875
- filtered: bfloat16 [1536, 1024], P('sp', 'tp'), may hold values from -1000 to 1000
- channel_gain: float32 [1024], P('tp'), may hold values from 0.1 to 1.9
- kernel_taps: float32 [31, 1024], P(None, 'tp'), may hold values from -1 to 1
- value_branch: bfloat16 [1536, 1024], P('sp', 'tp'), may hold values from -6 to 6
- gate_branch: bfloat16 [1536, 1024], P('sp', 'tp'), may hold values from -6 to 6
Outputs:
- gradient_value: bfloat16 [1536, 1024], P('sp', 'tp')
- gradient_gating: bfloat16 [1536, 1024], P('sp', 'tp')
- gradient_mixer: float32 [2048, 1024], P('sp', 'tp')
- gradient_gate: float32 [8, 2048, 1024], P('sp', None, 'tp')
- gradient_up: float32 [8, 2048, 1024], P('sp', None, 'tp')
- gradient_down: float32 [8, 1024, 2048], P('sp', 'tp')
The draws below stay inside these ranges and needn't reach their ends.
Inputs may be any that keep to these rules, and one draw needn't show every extreme that they name: `expert_ids`: the two experts of a token differ. Among the rows of one index of sp, at most 60 routes name the same expert, and in every draw some expert is named by exactly 60 of them.
All inputs are finite; a program needn't handle non-finite values.
Results may differ from the reference program's by a relative error of at most 0.012.
Values may be sent and summed in bfloat16 or wider, within the bound.
A program may use at most 64 MiB of HBM per device.

```python
import math
import jax
import jax.numpy as jnp
import numpy as np
from jax import lax

D = 2048
C = 1024
F = 1024
K = 31
TOK_DEV = 192
TOKENS = 1536
EXPERTS = 8
CAP = 60
N_SP = 8
N_TP = 4


def draw_filtered(key, part):
    keys = jax.random.split(jax.random.fold_in(key, 17), 3)
    jitter = jax.random.uniform(keys[0], (C,), jnp.float32, 0.0, 1.0)
    channel_scale = jnp.exp(jnp.log(10.0) * (jnp.arange(C, dtype=jnp.float32) + jitter * C / 4.0) / (1.25 * C))
    row_scale = jnp.exp(jax.random.uniform(keys[1], (TOKENS, 1), jnp.float32, 0.0, jnp.log(10.0)))
    values = jax.random.normal(keys[2], (TOKENS, C), jnp.float32) * channel_scale * row_scale
    return jnp.clip(values, -1000.0, 1000.0).astype(jnp.bfloat16)


def strengthened(array, stream_key, source, target, parts, factor):
    owner, partner = [(jnp.arange(array.shape[dim]) // (array.shape[dim] // parts)).reshape([-1 if axis == dim else 1 for axis in range(array.ndim)]) for dim in (source, target)]
    chosen = jax.random.permutation(stream_key, parts)[partner]
    strong = (owner == chosen) | (owner == (partner + parts // 2) % parts)
    return jnp.where(strong, factor * array, array)


def level_of(key, shape, cuts, low, top_value):
    gain, own = 1.0, jax.random.fold_in(key, 6)
    for axis_at, blocks in cuts:
        draws = jnp.exp(jax.random.uniform(jax.random.fold_in(own, axis_at), (blocks,), jnp.float32, low / len(cuts), top_value / len(cuts)))
        gain = gain * jnp.repeat(draws, shape[axis_at] // blocks).reshape([-1 if axis == axis_at else 1 for axis in range(len(shape))])
    return gain


def shared_out(own_key, own, number, rows, number_of, top, limit, slope):
    ranking = jax.random.permutation(own_key, number_of)
    heavy_load, ordinary = load_shares(number_of, rows * top, limit, slope, True), load_shares(number_of, rows * top, limit, slope, False)
    places = jnp.arange(number_of)

    def named(sizes, offset_by):
        used = int((sizes > 0).sum())
        fixed = max(1, used // 4)
        shifted = fixed + (places - fixed + offset_by * (used - fixed)) % max(1, number_of - fixed)
        return jnp.zeros((number_of,), jnp.int32).at[ranking[jnp.where(places < fixed, places, shifted)]].set(jnp.asarray(sizes, jnp.int32))

    sizes = jnp.where(number % 4 == 0, named(heavy_load, number // 4), named(ordinary, number - number // 4 - 1))
    mixed = jax.random.permutation(jax.random.fold_in(own, 3), number_of)
    giver, sink = mixed[0:number_of // 2 * 2:2], mixed[1:number_of // 2 * 2:2]
    room = jnp.minimum(sizes[giver] - 1, limit - sizes[sink]) // 2
    room = jnp.where((giver == ranking[0]) | (sink == ranking[0]) | (sizes[sink] == 0), 0, jnp.maximum(room, 0))
    shifted = jax.random.randint(jax.random.fold_in(own, 4), (number_of // 2,), 0, 1 << 20) % (room + 1)
    sizes = sizes.at[giver].add(-shifted).at[sink].add(shifted)
    items = jnp.searchsorted(jnp.cumsum(sizes), jnp.arange(rows * top), side="right").astype(jnp.int32)
    listing = items.reshape(top, rows).T
    listing = listing[jax.random.permutation(jax.random.fold_in(own, 1), rows)]
    offset_by = jax.random.randint(jax.random.fold_in(own, 2), (rows, 1), 0, top)
    return jnp.take_along_axis(listing, (jnp.arange(top)[None, :] + offset_by) % top, axis=1)


def load_shares(amount, total, reach, skew, full):
    weights = [(1 << 20) // math.isqrt(grade ** skew) + 1 for grade in range(1, amount + 1)]
    largest = reach if full else min(reach, max(-(-total // amount), total * weights[0] // sum(weights)))
    least = 1 if total - largest >= amount - 1 else 0
    holding, spare = [largest] + [least] * (amount - 1), total - largest - least * (amount - 1)
    while spare > 0:
        free = [i for i in range(1, amount) if holding[i] < largest] or [i for i in range(1, amount) if holding[i] < reach]
        mass, left = sum([weights[i] for i in free]), spare
        for i in free:
            addition = min(reach - holding[i], max(1, left * weights[i] // mass), spare)
            holding[i] = holding[i] + addition
            spare = spare - addition
    return np.array(holding)


def noise(rng, shape, width, limit, cuts=(), held_as=jnp.bfloat16):
    values = width * jax.random.normal(rng, shape, jnp.float32)
    if cuts:
        values = values * level_of(rng, shape, cuts, -0.22, 0.18)
    return jnp.clip(values, -limit, limit).astype(held_as)


def gaussian_with(stream_key, shape, deviation, bound, shards, heavy, kind=jnp.bfloat16):
    array = deviation * jax.random.normal(stream_key, shape, jnp.float32)
    if shards:
        array = array * level_of(stream_key, shape, shards, -0.22, 0.18)
    return jnp.clip(strengthened(array, jax.random.fold_in(stream_key, 3), *heavy), -bound, bound).astype(kind)


def setup_inputs(seed: int = 0) -> dict:
    key_of = jax.random.split(jax.random.key(seed), 16)
    stream = noise(key_of[0], (TOKENS, D), 1.0, 6.0, ((0, 8),))
    upstream = gaussian_with(key_of[1], (TOKENS, D), 1.0, 6.0, ((0, 8),), (0, 1, 8, 2.0))
    expert_gain = jnp.clip(1.0 + 0.18 * jax.random.normal(key_of[2], (D,), jnp.float32), 0.1, 1.9)
    expert_ids_keys = jax.random.split(jax.random.fold_in(key_of[3], 1), TOKENS // TOK_DEV)
    expert_ids_turns = jax.random.permutation(jax.random.fold_in(key_of[3], 3), TOKENS // TOK_DEV)
    expert_ids = jax.vmap(lambda own, number: shared_out(jax.random.fold_in(key_of[3], 2), own, number, TOK_DEV, EXPERTS, 2, CAP, 1))(expert_ids_keys, expert_ids_turns).reshape((TOKENS, 2))
    group_weight = jnp.clip(0.25 + 0.75 * jax.random.uniform(key_of[4], (TOKENS,), jnp.float32) ** level_of(key_of[4], (TOKENS,), ((0, 8),), -0.2, 0.2), 0.25, 1.0)
    pair_scores = noise(key_of[5], (TOKENS, 2), 1.5, 6.0, ((0, 8),), jnp.float32)
    gate_weight = noise(key_of[6], (EXPERTS, D, F), D ** -0.5, 0.125, ((0, 8), (2, 4)))
    up_weight = noise(key_of[7], (EXPERTS, D, F), D ** -0.5, 0.125, ((0, 8), (2, 4)))
    down_weight = noise(key_of[8], (EXPERTS, F, D), F ** -0.5, 0.1875, ((0, 8), (1, 4)))
    mixer_weight = noise(key_of[9], (C, D), C ** -0.5, 0.1875, ((0, 4),))
    filtered = draw_filtered(jax.random.fold_in(key_of[15], 71), 0)
    channel_gain = jnp.clip(1.0 + 0.18 * jax.random.normal(key_of[11], (C,), jnp.float32), 0.1, 1.9)
    kernel_taps = noise(key_of[12], (K, C), K ** -0.5, 1.0, ((1, 4),), jnp.float32)
    value_branch = noise(key_of[13], (TOKENS, C), 1.0, 6.0, ((0, 8), (1, 4)))
    gate_branch = noise(key_of[14], (TOKENS, C), 1.5, 6.0, ((0, 8), (1, 4)))
    return dict(stream=stream, upstream=upstream, expert_gain=expert_gain, expert_ids=expert_ids, group_weight=group_weight, pair_scores=pair_scores, gate_weight=gate_weight, up_weight=up_weight, down_weight=down_weight, mixer_weight=mixer_weight, filtered=filtered, channel_gain=channel_gain, kernel_taps=kernel_taps, value_branch=value_branch, gate_branch=gate_branch)


EPS = 1e-06

def route_slots(routes, capacity, experts):
    flat = routes.reshape(-1)
    onehot = (flat[:, None] == jnp.arange(experts, dtype=jnp.int32)[None, :]).astype(jnp.int32)
    before = jnp.cumsum(onehot, axis=0) - onehot
    position = lax.optimization_barrier(jnp.sum(before * onehot, axis=1))
    slots = (flat * capacity + position).astype(jnp.int32)
    total = flat.shape[0]
    source = jnp.full((experts * capacity,), total, jnp.int32).at[slots].set(jnp.arange(total, dtype=jnp.int32))
    return (slots, source)

def silu_slope(value, sigma):
    return sigma * (1.0 + value * (1.0 - sigma))

def reference(stream, upstream, expert_gain, expert_ids, group_weight, pair_scores, gate_weight, up_weight, down_weight, mixer_weight, filtered, channel_gain, kernel_taps, value_branch, gate_branch):
    stream_f = stream.astype(jnp.float32)
    inv_rms = lax.rsqrt(lax.optimization_barrier(jnp.mean(stream_f * stream_f, axis=1, keepdims=True)) + EPS)
    normed = (stream_f * inv_rms * expert_gain).astype(jnp.bfloat16)
    spread = pair_scores[:, 0] - pair_scores[:, 1]
    route_weight = group_weight[:, None] * jnp.stack([jax.nn.sigmoid(spread), jax.nn.sigmoid(-spread)], axis=1)
    per_block = expert_ids.reshape(N_SP, TOK_DEV, 2)
    slots, source = jax.vmap(lambda routes: route_slots(routes, CAP, EXPERTS))(per_block)
    routes_dev = 2 * TOK_DEV
    offsets = (jnp.arange(N_SP, dtype=jnp.int32) * routes_dev)[:, None]
    global_source = jnp.where(source < routes_dev, source + offsets, 2 * TOKENS).astype(jnp.int32)
    table = global_source.reshape(N_SP, EXPERTS, CAP).transpose(1, 0, 2).reshape(EXPERTS, N_SP * CAP)
    normed_ext = jnp.concatenate([normed, jnp.zeros((1, D), jnp.bfloat16)], axis=0)
    upstream_ext = jnp.concatenate([upstream, jnp.zeros((1, D), jnp.bfloat16)], axis=0)
    weight_ext = jnp.concatenate([route_weight.reshape(-1), jnp.zeros((1,), jnp.float32)], axis=0)
    block = F // N_TP

    def one_expert(args):
        index, gate_w, up_w, down_w = args
        token_index = index // 2
        rows = normed_ext[token_index]
        cots = (weight_ext[index][:, None] * upstream_ext[token_index].astype(jnp.float32)).astype(jnp.bfloat16)
        pre_gate = jnp.dot(rows, gate_w, preferred_element_type=jnp.float32)
        pre_up = jnp.dot(rows, up_w, preferred_element_type=jnp.float32)
        sigma = jax.nn.sigmoid(pre_gate)
        silu_gate = pre_gate * sigma
        hidden = (silu_gate * pre_up).astype(jnp.bfloat16)
        grad_hidden = jnp.dot(cots, down_w.T, preferred_element_type=jnp.float32)
        grad_pre_gate = (grad_hidden * pre_up * silu_slope(pre_gate, sigma)).astype(jnp.bfloat16)
        grad_pre_up = (grad_hidden * silu_gate).astype(jnp.bfloat16)
        grad_gate_w = jnp.dot(rows.T, grad_pre_gate, preferred_element_type=jnp.float32)
        grad_up_w = jnp.dot(rows.T, grad_pre_up, preferred_element_type=jnp.float32)
        grad_down_w = jnp.dot(hidden.T, cots, preferred_element_type=jnp.float32)
        terms = jnp.einsum('rtf,dtf->trd', grad_pre_gate.reshape(-1, N_TP, block).astype(jnp.float32), gate_w.reshape(D, N_TP, block).astype(jnp.float32))
        terms = terms + jnp.einsum('rtf,dtf->trd', grad_pre_up.reshape(-1, N_TP, block).astype(jnp.float32), up_w.reshape(D, N_TP, block).astype(jnp.float32))
        rounded = lax.optimization_barrier(terms.astype(jnp.bfloat16))
        returned = lax.optimization_barrier(jnp.sum(rounded.astype(jnp.float32), axis=0)).astype(jnp.bfloat16)
        return (grad_gate_w, grad_up_w, grad_down_w, returned)
    gradient_gate, gradient_up, gradient_down, returned = lax.map(one_expert, (table, gate_weight, up_weight, down_weight))
    returned_flat = returned.reshape(EXPERTS * N_SP * CAP, D)
    expert_of = slots // CAP
    position = slots % CAP
    flat_index = (expert_of * (N_SP * CAP) + jnp.arange(N_SP, dtype=jnp.int32)[:, None] * CAP + position).astype(jnp.int32).reshape(TOKENS, 2)
    grad_normed = returned_flat[flat_index[:, 0]].astype(jnp.float32) + returned_flat[flat_index[:, 1]].astype(jnp.float32)
    weighted = grad_normed * expert_gain
    inner = lax.optimization_barrier(jnp.mean(weighted * stream_f, axis=1, keepdims=True))
    grad_stream = (upstream.astype(jnp.float32) + inv_rms * weighted - stream_f * inv_rms * inv_rms * inv_rms * inner).astype(jnp.bfloat16)
    grad_act = jnp.dot(grad_stream, mixer_weight.T, preferred_element_type=jnp.float32)
    filt = filtered.astype(jnp.float32)
    mean_c = lax.optimization_barrier(jnp.mean(filt, axis=1, keepdims=True))
    raw = filt - mean_c
    inv_std = lax.rsqrt(lax.optimization_barrier(jnp.mean(raw * raw, axis=1, keepdims=True)) + EPS)
    centred = raw * inv_std
    normal_out = centred * channel_gain
    sigma = jax.nn.sigmoid(normal_out)
    activated = (normal_out * sigma).astype(jnp.bfloat16)
    gradient_mixer = jnp.dot(grad_stream.T, activated, preferred_element_type=jnp.float32)
    grad_centred = grad_act * silu_slope(normal_out, sigma) * channel_gain
    first_mean = lax.optimization_barrier(jnp.mean(grad_centred, axis=1, keepdims=True))
    second_mean = lax.optimization_barrier(jnp.mean(grad_centred * centred, axis=1, keepdims=True))
    grad_filtered = (inv_std * (grad_centred - first_mean - centred * second_mean)).astype(jnp.bfloat16)
    extended = jnp.concatenate([grad_filtered.astype(jnp.float32), jnp.zeros((K - 1, C), jnp.float32)], axis=0)
    grad_mixed = lax.conv_general_dilated(extended[None], kernel_taps[::-1][:, None, :], (1,), 'VALID', dimension_numbers=('NWC', 'WIO', 'NWC'), feature_group_count=C, precision=lax.Precision.HIGHEST)[0]
    sig_gate = jax.nn.sigmoid(gate_branch.astype(jnp.float32))
    gradient_value = (grad_mixed * sig_gate).astype(jnp.bfloat16)
    gradient_gating = (grad_mixed * value_branch.astype(jnp.float32) * sig_gate * (1.0 - sig_gate)).astype(jnp.bfloat16)
    return (gradient_value, gradient_gating, gradient_mixer, gradient_gate, gradient_up, gradient_down)
```

```python
import functools

import jax
import jax.numpy as jnp
from jax import lax
from jax.experimental import pallas as pl
from jax.experimental.pallas import tpu as pltpu
from jax.sharding import PartitionSpec as P

EPS = 1e-06
MESH = pl.DeviceIdType.MESH
F32 = jnp.float32
BF16 = jnp.bfloat16
HIGHEST = lax.Precision.HIGHEST


def silu_slope(value, sigma):
    return sigma * (1.0 + value * (1.0 - sigma))


def contract_last(left, right, precision=None):
    return lax.dot_general(
        left, right, (((1,), (1,)), ((), ())), preferred_element_type=F32, precision=precision
    )


def contract_first(left, right):
    return lax.dot_general(left, right, (((0,), (0,)), ((), ())), preferred_element_type=F32)


def round_up(value, unit):
    return -(-value // unit) * unit


def flip(index, mask):
    bit = 1
    while bit <= mask:
        if mask & bit:
            index = index + bit - 2 * bit * ((index // bit) % 2)
        bit *= 2
    return index


def low_bit(mask):
    return mask & -mask


def bits_below(limit):
    found, bit = [], 1
    while bit < limit:
        found.append(bit)
        bit *= 2
    return found[::-1]


def remote(src, dst, send, recv, where):
    return pltpu.make_async_remote_copy(
        src_ref=src, dst_ref=dst, send_sem=send, recv_sem=recv, device_id=where, device_id_type=MESH
    )


def enter(me, n, tp, groups):
    barrier = pltpu.get_barrier_semaphore()

    def greet(i, carry):
        pl.semaphore_signal(
            barrier, inc=1, device_id={"sp": lax.rem(me + i, n)}, device_id_type=MESH
        )
        return carry

    lax.fori_loop(1, n, greet, 0)
    for bit in bits_below(groups):
        pl.semaphore_signal(barrier, inc=1, device_id={"tp": flip(tp, bit)}, device_id_type=MESH)
    pl.semaphore_wait(barrier, n - 1 + len(bits_below(groups)))


class Spread:
    def __init__(self, place, tp, groups, send, recv):
        self.place, self.tp, self.groups = place, tp, groups
        self.send_sem, self.recv_sem = send, recv

    def copy(self, mask, bit):
        ref = self.place(flip(self.tp, mask))
        return remote(
            ref,
            ref,
            self.send_sem(mask | bit),
            self.recv_sem(mask | bit),
            {"tp": flip(self.tp, bit)},
        )

    def wait(self, mask):
        ref = self.place(flip(self.tp, mask))
        where = {"tp": flip(self.tp, low_bit(mask))}
        remote(ref, ref, self.send_sem(mask), self.recv_sem(mask), where).wait_recv()

    def begin(self):
        for bit in bits_below(self.groups):
            self.copy(0, bit).start()

    def masks(self):
        return sorted(range(1, self.groups), key=lambda m: (bin(m).count("1"), -low_bit(m)))

    def relay(self):
        for mask in self.masks():
            onward = bits_below(low_bit(mask))
            if onward:
                self.wait(mask)
                for bit in onward:
                    self.copy(mask, bit).start()

    def finish(self):
        for mask in self.masks():
            if not bits_below(low_bit(mask)):
                self.wait(mask)
        for mask in range(1, self.groups):
            self.copy(mask - low_bit(mask), low_bit(mask)).wait_send()


def each(first, last, step):
    def run(i, carry):
        step(i)
        return carry

    lax.fori_loop(first, last, run, 0)


def dispatch_kernel(
    n,
    groups,
    pcap,
    stream,
    upstream,
    gain,
    ids,
    weight,
    scores,
    filtered,
    rows,
    cots,
    places,
    stats,
    send_rows,
    send_cots,
    sp_send,
    sp_recv,
    tp_send,
    tp_recv,
    st_send,
    st_recv,
):
    me, tp = lax.axis_index("sp"), lax.axis_index("tp")
    tokens, width = stream.shape
    column = width // groups
    enter(me, n, tp, groups)

    filt = filtered[...]
    square = filt.astype(F32) * filt.astype(F32)
    high = square.astype(BF16)
    low = (square - high.astype(F32)).astype(BF16)
    ones = jnp.ones((8, filt.shape[1]), BF16)
    total = contract_last(ones, filt)
    total_square = contract_last(ones, high) + contract_last(ones, low)
    line = lax.broadcasted_iota(jnp.int32, total.shape, 0)
    stats[tp] = jnp.where(line == 0, total, total_square)
    sums = Spread(
        lambda o: stats.at[o], tp, groups, lambda m: st_send.at[m], lambda m: st_recv.at[m]
    )
    sums.begin()

    routes = 2 * tokens
    onehot = (lax.broadcasted_iota(jnp.int32, (n, routes), 0) == ids[...]).astype(F32)
    earlier = (
        lax.broadcasted_iota(jnp.int32, (routes, routes), 0)
        < lax.broadcasted_iota(jnp.int32, (routes, routes), 1)
    ).astype(F32).astype(BF16)
    before = jnp.dot(onehot.astype(BF16), earlier, preferred_element_type=F32)
    base = (lax.broadcasted_iota(jnp.int32, (n, routes), 0) * pcap).astype(F32)
    slot = jnp.sum(onehot * (before + base), axis=0, keepdims=True).astype(jnp.int32)
    slot_at = lax.broadcasted_iota(jnp.int32, (n * pcap, tokens), 0)
    first = (slot_at == slot[:, :tokens]).astype(F32).astype(BF16)
    second = (slot_at == slot[:, tokens:]).astype(F32).astype(BF16)
    both = first + second
    places[...] = both

    stream_f = stream[...].astype(F32)
    inv_rms = lax.rsqrt(jnp.mean(stream_f * stream_f, axis=1, keepdims=True) + EPS)
    cols = pl.ds(pl.multiple_of(tp * column, column), column)
    normed = (stream[:, cols].astype(F32) * inv_rms * gain[:, cols]).astype(BF16)
    send_rows[...] = jnp.dot(both, normed, preferred_element_type=F32).astype(BF16)
    spread = scores[:, 0:1] - scores[:, 1:2]
    up = upstream[:, cols].astype(F32)
    scaled_a = (weight[...] * jax.nn.sigmoid(spread) * up).astype(BF16)
    scaled_b = (weight[...] * jax.nn.sigmoid(-spread) * up).astype(BF16)
    send_cots[...] = (
        jnp.dot(first, scaled_a, preferred_element_type=F32)
        + jnp.dot(second, scaled_b, preferred_element_type=F32)
    ).astype(BF16)

    pairs = ((send_rows, rows), (send_cots, cots))

    def block(j):
        return pl.ds(pl.multiple_of(j * pcap, pcap), pcap)

    def place(full, s, o):
        return full.at[block(s), pl.ds(pl.multiple_of(o * column, column), column)]

    def sp_copy(a, i, j, s):
        src, full = pairs[a]
        return remote(
            src.at[block(j)], place(full, s, tp), sp_send.at[a, i], sp_recv.at[a, i], {"sp": j}
        )

    def send(i):
        for a in range(2):
            sp_copy(a, i, lax.rem(me + i, n), me).start()

    each(1, n, send)
    for src, full in pairs:
        full[block(me), cols] = src[block(me)]

    def gather(a, i):
        s = lax.rem(me + n - i, n)
        return Spread(
            lambda o: place(pairs[a][1], s, o),
            tp,
            groups,
            lambda m: tp_send.at[a, i, m],
            lambda m: tp_recv.at[a, i, m],
        )

    def arrive(i):
        for a in range(2):
            s = lax.rem(me + n - i, n)
            sp_copy(a, i, s, s).wait_recv()
            gather(a, i).begin()
            gather(a, i - 1).relay()

    for a in range(2):
        gather(a, 0).begin()
    each(1, n, arrive)
    for a in range(2):
        gather(a, n - 1).relay()
    sums.relay()
    sums.finish()

    def close(i):
        for a in range(2):
            gather(a, i).finish()

    each(0, n, close)

    def sent(i):
        for a in range(2):
            sp_copy(a, i, lax.rem(me + i, n), me).wait_send()

    each(1, n, sent)


def tail_kernel(
    n,
    groups,
    pcap,
    partial,
    places,
    stats,
    stream,
    upstream,
    gain,
    mixer,
    filtered,
    channel_gain,
    taps,
    value,
    gate,
    out_value,
    out_gating,
    out_mixer,
    halves,
    passing,
    keep,
    crossed,
    outgoing,
    back,
    grad_normed,
    grad_stream,
    staged,
    grad_all,
    act_all,
    slopes,
    halo_out,
    halo_in,
    ext,
    core_send,
    core_recv,
    x_send,
    x_recv,
    sp_send,
    sp_recv,
    gn_send,
    gn_recv,
    far_send,
    far_recv,
    near_send,
    near_recv,
    gs_send,
    gs_recv,
    ga_send,
    ga_recv,
    sl_send,
    sl_recv,
    halo_send,
    halo_recv,
):
    me, tp = lax.axis_index("sp"), lax.axis_index("tp")
    tokens, width = stream.shape
    column = width // groups
    channels = filtered.shape[1] * groups
    portion = tokens // groups
    db = width // n
    pdb = grad_all.shape[1]
    reach = taps.shape[0] - 1
    hpad = halo_in.shape[0]
    enter(me, n, tp, groups)

    def block(j):
        return pl.ds(pl.multiple_of(j * pcap, pcap), pcap)

    def quarter(q):
        return pl.ds(pl.multiple_of(q * column, column), column)

    mate = flip(tp, 1)
    half = groups // 2

    def chunk(i):
        return lax.rem(me + 1 + i, n)

    def core_copy(i, h):
        j = chunk(i)
        return remote(
            partial.at[block(j), quarter(lax.rem(mate, 2) + 2 * h)],
            halves.at[block(j), pl.ds(h * column, column)],
            core_send.at[i, h],
            core_recv.at[i, h],
            {"tp": mate},
        )

    def start_core(i):
        for h in range(half):
            core_copy(i, h).start()

    each(0, n, start_core)

    sums = stats[0]
    for o in range(1, groups):
        sums = sums + stats[o]
    eye = (
        lax.broadcasted_iota(jnp.int32, (tokens, tokens), 0)
        == lax.broadcasted_iota(jnp.int32, (tokens, tokens), 1)
    ).astype(F32)
    sums = contract_last(eye, sums, HIGHEST)
    mean_c = sums[:, 0:1] / channels
    variance = sums[:, 1:2] / channels - mean_c * mean_c
    inv_std = lax.rsqrt(variance + EPS)
    centred = (filtered[...].astype(F32) - mean_c) * inv_std
    normal_out = centred * channel_gain[...]
    sig_norm = jax.nn.sigmoid(normal_out)

    def act_rows(s):
        return pl.ds(pl.multiple_of(s * tokens, tokens), tokens)

    act_all[act_rows(me)] = (normal_out * sig_norm).astype(BF16)
    buddy = flip(me, 1)

    def far_copy(i, to, origin):
        ref = act_all.at[act_rows(origin)]
        return remote(ref, ref, far_send.at[i], far_recv.at[i], {"sp": to})

    def near_copy(i, holder):
        ref = act_all.at[act_rows(lax.rem(holder + n - 2 * i, n))]
        return remote(ref, ref, near_send.at[i], near_recv.at[i], {"sp": buddy})

    each(1, n // 2, lambda i: far_copy(i, lax.rem(me + 2 * i, n), me).start())
    near_copy(0, me).start()

    def x_copy(i, h):
        j = chunk(i)
        peer = lax.rem(tp, 2) + 2 * h
        ref = passing.at[block(j), pl.ds(h * column, column)]
        return peer, ref

    bits = [bit // 2 for bit in bits_below(groups) if bit > 1]
    mine = tp // 2

    def cross(i, m, wait):
        j = chunk(i)
        h = flip(mine, m)
        return remote(
            passing.at[block(j), pl.ds(pl.multiple_of(h * column, column), column)],
            crossed.at[block(j), pl.ds((m - 1) * column, column)],
            x_send.at[i, m],
            x_recv.at[i, m],
            {"tp": flip(tp, 2 * m)},
        )

    def add_core(i):
        j = chunk(i)
        for h in range(half):
            core_copy(i, h).wait_recv()
        for h in range(half):
            own = partial[block(j), quarter(lax.rem(tp, 2) + 2 * h)].astype(F32)
            passing[block(j), pl.ds(h * column, column)] = (
                own + halves[block(j), pl.ds(h * column, column)].astype(F32)
            ).astype(BF16)
        for m in range(1, half):
            cross(i, m, False).start()

    def home_copy(i, s):
        return remote(
            outgoing.at[block(chunk(i))],
            back.at[block(s)],
            sp_send.at[i],
            sp_recv.at[i],
            {"sp": chunk(i)},
        )

    def total_of(i):
        j = chunk(i)
        for m in range(1, half):
            cross(i, m, True).wait_recv()
        total = passing[block(j), pl.ds(pl.multiple_of(mine * column, column), column)].astype(F32)
        for m in range(1, half):
            total = total + crossed[block(j), pl.ds((m - 1) * column, column)].astype(F32)
        return total.astype(BF16)

    def add_x(i):
        outgoing[block(chunk(i))] = total_of(i)
        home_copy(i, me).start()

    add_core(0)

    def both(i):
        add_core(i)
        add_x(i - 1)

    each(1, n, both)
    back[block(me)] = total_of(n - 1)

    def relay_act(i):
        origin = lax.rem(me + n - 2 * i, n)
        far_copy(i, origin, origin).wait_recv()
        near_copy(i, me).start()

    each(1, n // 2, relay_act)

    inv_rms = jnp.zeros((tokens, 1), F32)
    for q in range(groups):
        piece = stream[:, q * column : (q + 1) * column].astype(F32)
        inv_rms = inv_rms + jnp.sum(piece * piece, axis=1, keepdims=True)
    inv_rms = lax.rsqrt(inv_rms / width + EPS)

    def came_home(i):
        s = lax.rem(me + n - 1 - i, n)
        home_copy(i, s).wait_recv()

    each(0, n - 1, came_home)
    grad_normed[:, quarter(tp)] = contract_first(places[...], back[...]).astype(BF16)
    gather = Spread(
        lambda o: grad_normed.at[:, quarter(o)],
        tp,
        groups,
        lambda m: gn_send.at[m],
        lambda m: gn_recv.at[m],
    )
    gather.begin()
    gather.relay()
    gather.finish()

    inner = jnp.zeros((tokens, 1), F32)
    for q in range(groups):
        at = slice(q * column, (q + 1) * column)
        weighted = grad_normed[:, at].astype(F32) * gain[:, at]
        inner = inner + jnp.sum(weighted * stream[:, at].astype(F32), axis=1, keepdims=True)
    inner = inv_rms * inv_rms * inv_rms * (inner / width)
    for q in range(groups):
        at = slice(q * column, (q + 1) * column)
        weighted = grad_normed[:, at].astype(F32) * gain[:, at]
        grad_stream[:, at] = (
            upstream[:, at].astype(F32) + inv_rms * weighted - stream[:, at].astype(F32) * inner
        ).astype(BF16)

    def part(s, o):
        start = pl.multiple_of(s * tokens + o * portion, portion)
        return grad_all.at[pl.ds(start, portion)]

    my_rows = pl.ds(pl.multiple_of(tp * portion, portion), portion)
    if db == pdb:

        def cut(j):
            return grad_stream.at[my_rows, pl.ds(pl.multiple_of(j * db, db), db)]

        grad_all[act_rows(me)] = grad_stream[:, pl.ds(pl.multiple_of(me * db, db), db)]
    else:

        def pick(j):
            where = lax.broadcasted_iota(jnp.int32, (width, pdb), 0)
            lane = lax.broadcasted_iota(jnp.int32, (width, pdb), 1)
            return ((where == lane + j * db) & (lane < db)).astype(F32).astype(BF16)

        def stage(j):
            staged[j] = jnp.dot(
                grad_stream[my_rows], pick(j), preferred_element_type=F32
            ).astype(BF16)

        each(0, n, stage)

        def cut(j):
            return staged.at[j]

        grad_all[act_rows(me)] = jnp.dot(
            grad_stream[...], pick(me), preferred_element_type=F32
        ).astype(BF16)

    def cut_copy(i, j, s):
        return remote(cut(j), part(s, tp), gs_send.at[i], gs_recv.at[i], {"sp": j})

    each(1, n, lambda i: cut_copy(i, lax.rem(me + i, n), me).start())

    grad_act = contract_last(grad_stream[...], mixer[...])
    grad_centred = grad_act * silu_slope(normal_out, sig_norm) * channel_gain[...]
    ones = jnp.ones((8, filtered.shape[1]), F32)
    slope_sum = contract_last(ones, grad_centred, HIGHEST)
    slope_cross = contract_last(ones, grad_centred * centred, HIGHEST)
    line = lax.broadcasted_iota(jnp.int32, slope_sum.shape, 0)
    slopes[tp] = jnp.where(line == 0, slope_sum, slope_cross)
    meet = Spread(
        lambda o: slopes.at[o], tp, groups, lambda m: sl_send.at[m], lambda m: sl_recv.at[m]
    )
    meet.begin()
    meet.relay()
    meet.finish()
    sums = slopes[0]
    for o in range(1, groups):
        sums = sums + slopes[o]
    sums = contract_last(eye, sums, HIGHEST)
    grad_filtered = (
        inv_std
        * (grad_centred - sums[:, 0:1] / channels - centred * (sums[:, 1:2] / channels))
    ).astype(BF16)
    halo_out[...] = grad_filtered[:hpad]
    ext[:tokens] = grad_filtered.astype(F32)

    def halo_copy():
        return remote(halo_out, halo_in, halo_send, halo_recv, {"sp": lax.rem(me + n - 1, n)})

    halo_copy().start()

    def spread_cut(i):
        s = lax.rem(me + n - i, n)
        return Spread(
            lambda o: part(s, o),
            tp,
            groups,
            lambda m: ga_send.at[i, m],
            lambda m: ga_recv.at[i, m],
        )

    def cut_arrives(i):
        s = lax.rem(me + n - i, n)
        cut_copy(i, s, s).wait_recv()
        spread_cut(i).begin()

    each(1, n, cut_arrives)

    halo_copy().wait_recv()
    inside = jnp.where(me < n - 1, 1.0, 0.0)
    ext[tokens:] = halo_in[...].astype(F32) * inside
    each(1, n, lambda i: spread_cut(i).relay())
    mixed = jnp.zeros((tokens, filtered.shape[1]), F32)
    for k in range(reach + 1):
        mixed = mixed + taps[k : k + 1] * ext[reach - k : reach - k + tokens]
    sig_gate = jax.nn.sigmoid(gate[...].astype(F32))
    out_value[...] = (mixed * sig_gate).astype(BF16)
    out_gating[...] = (mixed * value[...].astype(F32) * sig_gate * (1.0 - sig_gate)).astype(BF16)

    each(1, n, lambda i: spread_cut(i).finish())
    each(0, n // 2, lambda i: near_copy(i, buddy).wait_recv())
    out_mixer[...] = contract_first(grad_all[...], act_all[...])[:db]

    halo_copy().wait_send()
    each(1, n, lambda i: cut_copy(i, lax.rem(me + i, n), me).wait_send())
    each(1, n // 2, lambda i: far_copy(i, lax.rem(me + 2 * i, n), me).wait_send())
    each(0, n // 2, lambda i: near_copy(i, me).wait_send())
    each(0, n - 1, lambda i: home_copy(i, me).wait_send())

    def sums_sent(i):
        for h in range(half):
            core_copy(i, h).wait_send()
        for m in range(1, half):
            cross(i, m, True).wait_send()

    each(0, n, sums_sent)


def call(kernel, collective_id, outs, scratch, args):
    return pl.pallas_call(
        kernel,
        out_shape=outs,
        in_specs=[pl.BlockSpec(memory_space=pltpu.VMEM)] * len(args),
        out_specs=[pl.BlockSpec(memory_space=pltpu.VMEM)] * len(outs),
        scratch_shapes=scratch,
        compiler_params=pltpu.CompilerParams(
            collective_id=collective_id, has_side_effects=True, vmem_limit_bytes=40 << 20
        ),
    )(*args)


def body(
    stream,
    upstream,
    expert_gain,
    expert_ids,
    group_weight,
    pair_scores,
    gate_weight,
    up_weight,
    down_weight,
    mixer_weight,
    filtered,
    channel_gain,
    kernel_taps,
    value_branch,
    gate_branch,
):
    n, groups = lax.axis_size("sp"), lax.axis_size("tp")
    tokens, width = stream.shape
    capacity = max(2, 5 * tokens // (2 * n))
    pcap = round_up(capacity, 16)
    column = width // groups
    here = filtered.shape[1]
    slots = n * pcap
    dma = pltpu.SemaphoreType.DMA
    shape = jax.ShapeDtypeStruct
    gain = expert_gain[None]
    rows, cots, places, stats = call(
        functools.partial(dispatch_kernel, n, groups, pcap),
        0,
        [
            shape((slots, width), BF16),
            shape((slots, width), BF16),
            shape((slots, tokens), BF16),
            shape((groups, 8, tokens), F32),
        ],
        [
            pltpu.VMEM((slots, column), BF16),
            pltpu.VMEM((slots, column), BF16),
            dma((2, n)),
            dma((2, n)),
            dma((2, n, groups)),
            dma((2, n, groups)),
            dma((groups,)),
            dma((groups,)),
        ],
        (
            stream,
            upstream,
            gain,
            expert_ids.T.reshape(1, 2 * tokens),
            group_weight[:, None],
            pair_scores,
            filtered,
        ),
    )
    gate_local, up_local, down_local = gate_weight[0], up_weight[0], down_weight[0]
    pre_gate = jnp.dot(rows, gate_local, preferred_element_type=F32)
    pre_up = jnp.dot(rows, up_local, preferred_element_type=F32)
    sigma = jax.nn.sigmoid(pre_gate)
    silu_gate = pre_gate * sigma
    hidden = (silu_gate * pre_up).astype(BF16)
    grad_hidden = contract_last(cots, down_local)
    grad_pre_gate = (grad_hidden * pre_up * silu_slope(pre_gate, sigma)).astype(BF16)
    grad_pre_up = (grad_hidden * silu_gate).astype(BF16)
    partial = (
        contract_last(grad_pre_gate, gate_local) + contract_last(grad_pre_up, up_local)
    ).astype(BF16)
    gradient_gate = contract_first(rows, grad_pre_gate)[None]
    gradient_up = contract_first(rows, grad_pre_up)[None]
    gradient_down = contract_first(hidden, cots)[None]
    db = width // n
    pdb = round_up(db, 128)
    half = groups // 2
    hpad = round_up(kernel_taps.shape[0] - 1, 16)
    staged = (n, tokens // groups, pdb) if pdb != db else (1, 16, 128)
    gradient_value, gradient_gating, gradient_mixer = call(
        functools.partial(tail_kernel, n, groups, pcap),
        1,
        [
            shape((tokens, here), BF16),
            shape((tokens, here), BF16),
            shape((db, here), F32),
        ],
        [
            pltpu.VMEM((slots, half * column), BF16),
            pltpu.VMEM((slots, half * column), BF16),
            pltpu.VMEM((16, 128), F32),
            pltpu.VMEM((slots, max(1, half - 1) * column), BF16),
            pltpu.VMEM((slots, column), BF16),
            pltpu.VMEM((slots, column), BF16),
            pltpu.VMEM((tokens, width), BF16),
            pltpu.VMEM((tokens, width), BF16),
            pltpu.VMEM(staged, BF16),
            pltpu.VMEM((n * tokens, pdb), BF16),
            pltpu.VMEM((n * tokens, here), BF16),
            pltpu.VMEM((groups, 8, tokens), F32),
            pltpu.VMEM((hpad, here), BF16),
            pltpu.VMEM((hpad, here), BF16),
            pltpu.VMEM((tokens + hpad, here), F32),
            dma((n, half)),
            dma((n, half)),
            dma((n, half)),
            dma((n, half)),
            dma((n,)),
            dma((n,)),
            dma((groups,)),
            dma((groups,)),
            dma((n // 2,)),
            dma((n // 2,)),
            dma((n // 2,)),
            dma((n // 2,)),
            dma((n,)),
            dma((n,)),
            dma((n, groups)),
            dma((n, groups)),
            dma((groups,)),
            dma((groups,)),
            dma(()),
            dma(()),
        ],
        (
            partial,
            places,
            stats,
            stream,
            upstream,
            gain,
            mixer_weight,
            filtered,
            channel_gain[None],
            kernel_taps,
            value_branch,
            gate_branch,
        ),
    )
    return (
        gradient_value,
        gradient_gating,
        gradient_mixer,
        gradient_gate,
        gradient_up,
        gradient_down,
    )


def solution(mesh):
    return jax.shard_map(
        body,
        mesh=mesh,
        in_specs=(
            P("sp", None),
            P("sp", None),
            P(),
            P("sp", None),
            P("sp"),
            P("sp", None),
            P("sp", None, "tp"),
            P("sp", None, "tp"),
            P("sp", "tp", None),
            P("tp", None),
            P("sp", "tp"),
            P("tp"),
            P(None, "tp"),
            P("sp", "tp"),
            P("sp", "tp"),
        ),
        out_specs=(
            P("sp", "tp"),
            P("sp", "tp"),
            P("sp", "tp"),
            P("sp", None, "tp"),
            P("sp", None, "tp"),
            P("sp", "tp", None),
        ),
        check_vma=False,
    )
```

```python
import functools

import jax
import jax.numpy as jnp
from jax import lax
from jax.experimental import pallas as pl
from jax.experimental.pallas import tpu as pltpu
from jax.sharding import PartitionSpec as P

EPS = 1e-06
MESH = pl.DeviceIdType.MESH
F32 = jnp.float32
BF16 = jnp.bfloat16
HIGHEST = lax.Precision.HIGHEST


def silu_slope(value, sigma):
    return sigma * (1.0 + value * (1.0 - sigma))


def contract_last(left, right, precision=None):
    return lax.dot_general(
        left, right, (((1,), (1,)), ((), ())), preferred_element_type=F32, precision=precision
    )


def contract_first(left, right):
    return lax.dot_general(left, right, (((0,), (0,)), ((), ())), preferred_element_type=F32)


def round_up(value, unit):
    return -(-value // unit) * unit


def flip(index, mask):
    bit = 1
    while bit <= mask:
        if mask & bit:
            index = index + bit - 2 * bit * ((index // bit) % 2)
        bit *= 2
    return index


def low_bit(mask):
    return mask & -mask


def bits_below(limit):
    found, bit = [], 1
    while bit < limit:
        found.append(bit)
        bit *= 2
    return found[::-1]


def remote(src, dst, send, recv, where):
    return pltpu.make_async_remote_copy(
        src_ref=src, dst_ref=dst, send_sem=send, recv_sem=recv, device_id=where, device_id_type=MESH
    )


def enter(me, n, tp, groups):
    barrier = pltpu.get_barrier_semaphore()

    def greet(i, carry):
        pl.semaphore_signal(
            barrier, inc=1, device_id={"sp": lax.rem(me + i, n)}, device_id_type=MESH
        )
        return carry

    lax.fori_loop(1, n, greet, 0)
    for bit in bits_below(groups):
        pl.semaphore_signal(barrier, inc=1, device_id={"tp": flip(tp, bit)}, device_id_type=MESH)
    pl.semaphore_wait(barrier, n - 1 + len(bits_below(groups)))


class Spread:
    def __init__(self, place, tp, groups, send, recv):
        self.place, self.tp, self.groups = place, tp, groups
        self.send_sem, self.recv_sem = send, recv

    def copy(self, mask, bit):
        ref = self.place(flip(self.tp, mask))
        return remote(
            ref,
            ref,
            self.send_sem(mask | bit),
            self.recv_sem(mask | bit),
            {"tp": flip(self.tp, bit)},
        )

    def wait(self, mask):
        ref = self.place(flip(self.tp, mask))
        where = {"tp": flip(self.tp, low_bit(mask))}
        remote(ref, ref, self.send_sem(mask), self.recv_sem(mask), where).wait_recv()

    def begin(self):
        for bit in bits_below(self.groups):
            self.copy(0, bit).start()

    def masks(self):
        return sorted(range(1, self.groups), key=lambda m: (bin(m).count("1"), -low_bit(m)))

    def relay(self):
        for mask in self.masks():
            onward = bits_below(low_bit(mask))
            if onward:
                self.wait(mask)
                for bit in onward:
                    self.copy(mask, bit).start()

    def finish(self):
        for mask in self.masks():
            if not bits_below(low_bit(mask)):
                self.wait(mask)
        for mask in range(1, self.groups):
            self.copy(mask - low_bit(mask), low_bit(mask)).wait_send()


def each(first, last, step):
    def run(i, carry):
        step(i)
        return carry

    lax.fori_loop(first, last, run, 0)


def dispatch_kernel(
    n,
    groups,
    pcap,
    stream,
    upstream,
    gain,
    ids,
    weight,
    scores,
    filtered,
    rows,
    cots,
    places,
    stats,
    send_rows,
    send_cots,
    sp_send,
    sp_recv,
    tp_send,
    tp_recv,
    st_send,
    st_recv,
):
    me, tp = lax.axis_index("sp"), lax.axis_index("tp")
    tokens, width = stream.shape
    column = width // groups
    enter(me, n, tp, groups)

    filt = filtered[...]
    square = filt.astype(F32) * filt.astype(F32)
    high = square.astype(BF16)
    low = (square - high.astype(F32)).astype(BF16)
    ones = jnp.ones((8, filt.shape[1]), BF16)
    total = contract_last(ones, filt)
    total_square = contract_last(ones, high) + contract_last(ones, low)
    line = lax.broadcasted_iota(jnp.int32, total.shape, 0)
    stats[tp] = jnp.where(line == 0, total, total_square)
    sums = Spread(
        lambda o: stats.at[o], tp, groups, lambda m: st_send.at[m], lambda m: st_recv.at[m]
    )
    sums.begin()

    routes = 2 * tokens
    onehot = (lax.broadcasted_iota(jnp.int32, (n, routes), 0) == ids[...]).astype(F32)
    earlier = (
        lax.broadcasted_iota(jnp.int32, (routes, routes), 0)
        < lax.broadcasted_iota(jnp.int32, (routes, routes), 1)
    ).astype(F32).astype(BF16)
    before = jnp.dot(onehot.astype(BF16), earlier, preferred_element_type=F32)
    base = (lax.broadcasted_iota(jnp.int32, (n, routes), 0) * pcap).astype(F32)
    slot = jnp.sum(onehot * (before + base), axis=0, keepdims=True).astype(jnp.int32)
    slot_at = lax.broadcasted_iota(jnp.int32, (n * pcap, tokens), 0)
    first = (slot_at == slot[:, :tokens]).astype(F32).astype(BF16)
    second = (slot_at == slot[:, tokens:]).astype(F32).astype(BF16)
    both = first + second
    places[...] = both

    stream_f = stream[...].astype(F32)
    inv_rms = lax.rsqrt(jnp.mean(stream_f * stream_f, axis=1, keepdims=True) + EPS)
    cols = pl.ds(pl.multiple_of(tp * column, column), column)
    normed = (stream[:, cols].astype(F32) * inv_rms * gain[:, cols]).astype(BF16)
    send_rows[...] = jnp.dot(both, normed, preferred_element_type=F32).astype(BF16)
    spread = scores[:, 0:1] - scores[:, 1:2]
    up = upstream[:, cols].astype(F32)
    scaled_a = (weight[...] * jax.nn.sigmoid(spread) * up).astype(BF16)
    scaled_b = (weight[...] * jax.nn.sigmoid(-spread) * up).astype(BF16)
    send_cots[...] = (
        jnp.dot(first, scaled_a, preferred_element_type=F32)
        + jnp.dot(second, scaled_b, preferred_element_type=F32)
    ).astype(BF16)

    pairs = ((send_rows, rows), (send_cots, cots))

    def block(j):
        return pl.ds(pl.multiple_of(j * pcap, pcap), pcap)

    def place(full, s, o):
        return full.at[block(s), pl.ds(pl.multiple_of(o * column, column), column)]

    def sp_copy(a, i, j, s):
        src, full = pairs[a]
        return remote(
            src.at[block(j)], place(full, s, tp), sp_send.at[a, i], sp_recv.at[a, i], {"sp": j}
        )

    def send(i):
        for a in range(2):
            sp_copy(a, i, lax.rem(me + i, n), me).start()

    window = min(n - 1, 3)
    each(1, window + 1, send)
    for src, full in pairs:
        full[block(me), cols] = src[block(me)]

    def gather(a, i):
        s = lax.rem(me + n - i, n)
        return Spread(
            lambda o: place(pairs[a][1], s, o),
            tp,
            groups,
            lambda m: tp_send.at[a, i, m],
            lambda m: tp_recv.at[a, i, m],
        )

    def arrive(i):
        for a in range(2):
            s = lax.rem(me + n - i, n)
            sp_copy(a, i, s, s).wait_recv()
            if a == 0:
                pl.when(i + window < n)(lambda: send(i + window))
            gather(a, i).begin()
            gather(a, i - 1).relay()

    for a in range(2):
        gather(a, 0).begin()
    each(1, n, arrive)
    for a in range(2):
        gather(a, n - 1).relay()
    sums.relay()
    sums.finish()

    def close(i):
        for a in range(2):
            gather(a, i).finish()

    each(0, n, close)

    def sent(i):
        for a in range(2):
            sp_copy(a, i, lax.rem(me + i, n), me).wait_send()

    each(1, n, sent)


def tail_kernel(
    n,
    groups,
    pcap,
    partial,
    places,
    stats,
    stream,
    upstream,
    gain,
    mixer,
    filtered,
    channel_gain,
    taps,
    value,
    gate,
    out_value,
    out_gating,
    out_mixer,
    halves,
    passing,
    keep,
    crossed,
    outgoing,
    back,
    grad_normed,
    grad_stream,
    staged,
    grad_all,
    act_all,
    slopes,
    halo_out,
    halo_in,
    ext,
    core_send,
    core_recv,
    x_send,
    x_recv,
    sp_send,
    sp_recv,
    gn_send,
    gn_recv,
    far_send,
    far_recv,
    near_send,
    near_recv,
    gs_send,
    gs_recv,
    ga_send,
    ga_recv,
    sl_send,
    sl_recv,
    halo_send,
    halo_recv,
):
    me, tp = lax.axis_index("sp"), lax.axis_index("tp")
    tokens, width = stream.shape
    column = width // groups
    channels = filtered.shape[1] * groups
    portion = tokens // groups
    db = width // n
    pdb = grad_all.shape[1]
    reach = taps.shape[0] - 1
    hpad = halo_in.shape[0]
    enter(me, n, tp, groups)

    def block(j):
        return pl.ds(pl.multiple_of(j * pcap, pcap), pcap)

    def quarter(q):
        return pl.ds(pl.multiple_of(q * column, column), column)

    mate = flip(tp, 1)
    half = groups // 2

    def chunk(i):
        return lax.rem(me + 1 + i, n)

    def core_copy(i, h):
        j = chunk(i)
        return remote(
            partial.at[block(j), quarter(lax.rem(mate, 2) + 2 * h)],
            halves.at[block(j), pl.ds(h * column, column)],
            core_send.at[i, h],
            core_recv.at[i, h],
            {"tp": mate},
        )

    def start_core(i):
        for h in range(half):
            core_copy(i, h).start()

    each(0, n, start_core)

    sums = stats[0]
    for o in range(1, groups):
        sums = sums + stats[o]
    eye = (
        lax.broadcasted_iota(jnp.int32, (tokens, tokens), 0)
        == lax.broadcasted_iota(jnp.int32, (tokens, tokens), 1)
    ).astype(F32)
    sums = contract_last(eye, sums, HIGHEST)
    mean_c = sums[:, 0:1] / channels
    variance = sums[:, 1:2] / channels - mean_c * mean_c
    inv_std = lax.rsqrt(variance + EPS)
    centred = (filtered[...].astype(F32) - mean_c) * inv_std
    normal_out = centred * channel_gain[...]
    sig_norm = jax.nn.sigmoid(normal_out)

    def act_rows(s):
        return pl.ds(pl.multiple_of(s * tokens, tokens), tokens)

    act_all[act_rows(me)] = (normal_out * sig_norm).astype(BF16)
    buddy = flip(me, 1)

    def far_copy(i, to, origin):
        ref = act_all.at[act_rows(origin)]
        return remote(ref, ref, far_send.at[i], far_recv.at[i], {"sp": to})

    def near_copy(i, holder):
        ref = act_all.at[act_rows(lax.rem(holder + n - 2 * i, n))]
        return remote(ref, ref, near_send.at[i], near_recv.at[i], {"sp": buddy})

    each(1, n // 2, lambda i: far_copy(i, lax.rem(me + 2 * i, n), me).start())
    near_copy(0, me).start()

    def x_copy(i, h):
        j = chunk(i)
        peer = lax.rem(tp, 2) + 2 * h
        ref = passing.at[block(j), pl.ds(h * column, column)]
        return peer, ref

    bits = [bit // 2 for bit in bits_below(groups) if bit > 1]
    mine = tp // 2

    def cross(i, m, wait):
        j = chunk(i)
        h = flip(mine, m)
        return remote(
            passing.at[block(j), pl.ds(pl.multiple_of(h * column, column), column)],
            crossed.at[block(j), pl.ds((m - 1) * column, column)],
            x_send.at[i, m],
            x_recv.at[i, m],
            {"tp": flip(tp, 2 * m)},
        )

    def add_core(i):
        j = chunk(i)
        for h in range(half):
            core_copy(i, h).wait_recv()
        for h in range(half):
            own = partial[block(j), quarter(lax.rem(tp, 2) + 2 * h)].astype(F32)
            passing[block(j), pl.ds(h * column, column)] = (
                own + halves[block(j), pl.ds(h * column, column)].astype(F32)
            ).astype(BF16)
        for m in range(1, half):
            cross(i, m, False).start()

    def home_copy(i, s):
        return remote(
            outgoing.at[block(chunk(i))],
            back.at[block(s)],
            sp_send.at[i],
            sp_recv.at[i],
            {"sp": chunk(i)},
        )

    def total_of(i):
        j = chunk(i)
        for m in range(1, half):
            cross(i, m, True).wait_recv()
        total = passing[block(j), pl.ds(pl.multiple_of(mine * column, column), column)].astype(F32)
        for m in range(1, half):
            total = total + crossed[block(j), pl.ds((m - 1) * column, column)].astype(F32)
        return total.astype(BF16)

    def add_x(i):
        outgoing[block(chunk(i))] = total_of(i)
        home_copy(i, me).start()

    add_core(0)

    def both(i):
        add_core(i)
        add_x(i - 1)

    each(1, n, both)
    back[block(me)] = total_of(n - 1)

    def relay_act(i):
        origin = lax.rem(me + n - 2 * i, n)
        far_copy(i, origin, origin).wait_recv()
        near_copy(i, me).start()

    each(1, n // 2, relay_act)

    inv_rms = jnp.zeros((tokens, 1), F32)
    for q in range(groups):
        piece = stream[:, q * column : (q + 1) * column].astype(F32)
        inv_rms = inv_rms + jnp.sum(piece * piece, axis=1, keepdims=True)
    inv_rms = lax.rsqrt(inv_rms / width + EPS)

    def came_home(i):
        s = lax.rem(me + n - 1 - i, n)
        home_copy(i, s).wait_recv()

    each(0, n - 1, came_home)
    grad_normed[:, quarter(tp)] = contract_first(places[...], back[...]).astype(BF16)
    gather = Spread(
        lambda o: grad_normed.at[:, quarter(o)],
        tp,
        groups,
        lambda m: gn_send.at[m],
        lambda m: gn_recv.at[m],
    )
    gather.begin()
    gather.relay()
    gather.finish()

    inner = jnp.zeros((tokens, 1), F32)
    for q in range(groups):
        at = slice(q * column, (q + 1) * column)
        weighted = grad_normed[:, at].astype(F32) * gain[:, at]
        inner = inner + jnp.sum(weighted * stream[:, at].astype(F32), axis=1, keepdims=True)
    inner = inv_rms * inv_rms * inv_rms * (inner / width)
    for q in range(groups):
        at = slice(q * column, (q + 1) * column)
        weighted = grad_normed[:, at].astype(F32) * gain[:, at]
        grad_stream[:, at] = (
            upstream[:, at].astype(F32) + inv_rms * weighted - stream[:, at].astype(F32) * inner
        ).astype(BF16)

    def part(s, o):
        start = pl.multiple_of(s * tokens + o * portion, portion)
        return grad_all.at[pl.ds(start, portion)]

    my_rows = pl.ds(pl.multiple_of(tp * portion, portion), portion)
    if db == pdb:

        def cut(j):
            return grad_stream.at[my_rows, pl.ds(pl.multiple_of(j * db, db), db)]

        grad_all[act_rows(me)] = grad_stream[:, pl.ds(pl.multiple_of(me * db, db), db)]
    else:

        def pick(j):
            where = lax.broadcasted_iota(jnp.int32, (width, pdb), 0)
            lane = lax.broadcasted_iota(jnp.int32, (width, pdb), 1)
            return ((where == lane + j * db) & (lane < db)).astype(F32).astype(BF16)

        def stage(j):
            staged[j] = jnp.dot(
                grad_stream[my_rows], pick(j), preferred_element_type=F32
            ).astype(BF16)

        each(0, n, stage)

        def cut(j):
            return staged.at[j]

        grad_all[act_rows(me)] = jnp.dot(
            grad_stream[...], pick(me), preferred_element_type=F32
        ).astype(BF16)

    def cut_copy(i, j, s):
        return remote(cut(j), part(s, tp), gs_send.at[i], gs_recv.at[i], {"sp": j})

    each(1, n, lambda i: cut_copy(i, lax.rem(me + i, n), me).start())

    grad_act = contract_last(grad_stream[...], mixer[...])
    grad_centred = grad_act * silu_slope(normal_out, sig_norm) * channel_gain[...]
    ones = jnp.ones((8, filtered.shape[1]), F32)
    slope_sum = contract_last(ones, grad_centred, HIGHEST)
    slope_cross = contract_last(ones, grad_centred * centred, HIGHEST)
    line = lax.broadcasted_iota(jnp.int32, slope_sum.shape, 0)
    slopes[tp] = jnp.where(line == 0, slope_sum, slope_cross)
    meet = Spread(
        lambda o: slopes.at[o], tp, groups, lambda m: sl_send.at[m], lambda m: sl_recv.at[m]
    )
    meet.begin()
    meet.relay()
    meet.finish()
    sums = slopes[0]
    for o in range(1, groups):
        sums = sums + slopes[o]
    sums = contract_last(eye, sums, HIGHEST)
    grad_filtered = (
        inv_std
        * (grad_centred - sums[:, 0:1] / channels - centred * (sums[:, 1:2] / channels))
    ).astype(BF16)
    halo_out[...] = grad_filtered[:hpad]
    ext[:tokens] = grad_filtered.astype(F32)

    def halo_copy():
        return remote(halo_out, halo_in, halo_send, halo_recv, {"sp": lax.rem(me + n - 1, n)})

    halo_copy().start()

    def spread_cut(i):
        s = lax.rem(me + n - i, n)
        return Spread(
            lambda o: part(s, o),
            tp,
            groups,
            lambda m: ga_send.at[i, m],
            lambda m: ga_recv.at[i, m],
        )

    def cut_arrives(i):
        s = lax.rem(me + n - i, n)
        cut_copy(i, s, s).wait_recv()
        spread_cut(i).begin()

    each(1, n, cut_arrives)

    halo_copy().wait_recv()
    inside = jnp.where(me < n - 1, 1.0, 0.0)
    ext[tokens:] = halo_in[...].astype(F32) * inside
    each(1, n, lambda i: spread_cut(i).relay())
    mixed = jnp.zeros((tokens, filtered.shape[1]), F32)
    for k in range(reach + 1):
        mixed = mixed + taps[k : k + 1] * ext[reach - k : reach - k + tokens]
    sig_gate = jax.nn.sigmoid(gate[...].astype(F32))
    out_value[...] = (mixed * sig_gate).astype(BF16)
    out_gating[...] = (mixed * value[...].astype(F32) * sig_gate * (1.0 - sig_gate)).astype(BF16)

    each(1, n, lambda i: spread_cut(i).finish())
    each(0, n // 2, lambda i: near_copy(i, buddy).wait_recv())
    out_mixer[...] = contract_first(grad_all[...], act_all[...])[:db]

    halo_copy().wait_send()
    each(1, n, lambda i: cut_copy(i, lax.rem(me + i, n), me).wait_send())
    each(1, n // 2, lambda i: far_copy(i, lax.rem(me + 2 * i, n), me).wait_send())
    each(0, n // 2, lambda i: near_copy(i, me).wait_send())
    each(0, n - 1, lambda i: home_copy(i, me).wait_send())

    def sums_sent(i):
        for h in range(half):
            core_copy(i, h).wait_send()
        for m in range(1, half):
            cross(i, m, True).wait_send()

    each(0, n, sums_sent)


def call(kernel, collective_id, outs, scratch, args):
    return pl.pallas_call(
        kernel,
        out_shape=outs,
        in_specs=[pl.BlockSpec(memory_space=pltpu.VMEM)] * len(args),
        out_specs=[pl.BlockSpec(memory_space=pltpu.VMEM)] * len(outs),
        scratch_shapes=scratch,
        compiler_params=pltpu.CompilerParams(
            collective_id=collective_id, has_side_effects=True, vmem_limit_bytes=40 << 20
        ),
    )(*args)


def body(
    stream,
    upstream,
    expert_gain,
    expert_ids,
    group_weight,
    pair_scores,
    gate_weight,
    up_weight,
    down_weight,
    mixer_weight,
    filtered,
    channel_gain,
    kernel_taps,
    value_branch,
    gate_branch,
):
    n, groups = lax.axis_size("sp"), lax.axis_size("tp")
    tokens, width = stream.shape
    capacity = max(2, 5 * tokens // (2 * n))
    pcap = round_up(capacity, 16)
    column = width // groups
    here = filtered.shape[1]
    slots = n * pcap
    dma = pltpu.SemaphoreType.DMA
    shape = jax.ShapeDtypeStruct
    gain = expert_gain[None]
    rows, cots, places, stats = call(
        functools.partial(dispatch_kernel, n, groups, pcap),
        0,
        [
            shape((slots, width), BF16),
            shape((slots, width), BF16),
            shape((slots, tokens), BF16),
            shape((groups, 8, tokens), F32),
        ],
        [
            pltpu.VMEM((slots, column), BF16),
            pltpu.VMEM((slots, column), BF16),
            dma((2, n)),
            dma((2, n)),
            dma((2, n, groups)),
            dma((2, n, groups)),
            dma((groups,)),
            dma((groups,)),
        ],
        (
            stream,
            upstream,
            gain,
            expert_ids.T.reshape(1, 2 * tokens),
            group_weight[:, None],
            pair_scores,
            filtered,
        ),
    )
    gate_local, up_local, down_local = gate_weight[0], up_weight[0], down_weight[0]
    pre_gate = jnp.dot(rows, gate_local, preferred_element_type=F32)
    pre_up = jnp.dot(rows, up_local, preferred_element_type=F32)
    sigma = jax.nn.sigmoid(pre_gate)
    silu_gate = pre_gate * sigma
    hidden = (silu_gate * pre_up).astype(BF16)
    grad_hidden = contract_last(cots, down_local)
    grad_pre_gate = (grad_hidden * pre_up * silu_slope(pre_gate, sigma)).astype(BF16)
    grad_pre_up = (grad_hidden * silu_gate).astype(BF16)
    partial = (
        contract_last(grad_pre_gate, gate_local) + contract_last(grad_pre_up, up_local)
    ).astype(BF16)
    gradient_gate = contract_first(rows, grad_pre_gate)[None]
    gradient_up = contract_first(rows, grad_pre_up)[None]
    gradient_down = contract_first(hidden, cots)[None]
    db = width // n
    pdb = round_up(db, 128)
    half = groups // 2
    hpad = round_up(kernel_taps.shape[0] - 1, 16)
    staged = (n, tokens // groups, pdb) if pdb != db else (1, 16, 128)
    gradient_value, gradient_gating, gradient_mixer = call(
        functools.partial(tail_kernel, n, groups, pcap),
        1,
        [
            shape((tokens, here), BF16),
            shape((tokens, here), BF16),
            shape((db, here), F32),
        ],
        [
            pltpu.VMEM((slots, half * column), BF16),
            pltpu.VMEM((slots, half * column), BF16),
            pltpu.VMEM((16, 128), F32),
            pltpu.VMEM((slots, max(1, half - 1) * column), BF16),
            pltpu.VMEM((slots, column), BF16),
            pltpu.VMEM((slots, column), BF16),
            pltpu.VMEM((tokens, width), BF16),
            pltpu.VMEM((tokens, width), BF16),
            pltpu.VMEM(staged, BF16),
            pltpu.VMEM((n * tokens, pdb), BF16),
            pltpu.VMEM((n * tokens, here), BF16),
            pltpu.VMEM((groups, 8, tokens), F32),
            pltpu.VMEM((hpad, here), BF16),
            pltpu.VMEM((hpad, here), BF16),
            pltpu.VMEM((tokens + hpad, here), F32),
            dma((n, half)),
            dma((n, half)),
            dma((n, half)),
            dma((n, half)),
            dma((n,)),
            dma((n,)),
            dma((groups,)),
            dma((groups,)),
            dma((n // 2,)),
            dma((n // 2,)),
            dma((n // 2,)),
            dma((n // 2,)),
            dma((n,)),
            dma((n,)),
            dma((n, groups)),
            dma((n, groups)),
            dma((groups,)),
            dma((groups,)),
            dma(()),
            dma(()),
        ],
        (
            partial,
            places,
            stats,
            stream,
            upstream,
            gain,
            mixer_weight,
            filtered,
            channel_gain[None],
            kernel_taps,
            value_branch,
            gate_branch,
        ),
    )
    return (
        gradient_value,
        gradient_gating,
        gradient_mixer,
        gradient_gate,
        gradient_up,
        gradient_down,
    )


def solution(mesh):
    return jax.shard_map(
        body,
        mesh=mesh,
        in_specs=(
            P("sp", None),
            P("sp", None),
            P(),
            P("sp", None),
            P("sp"),
            P("sp", None),
            P("sp", None, "tp"),
            P("sp", None, "tp"),
            P("sp", "tp", None),
            P("tp", None),
            P("sp", "tp"),
            P("tp"),
            P(None, "tp"),
            P("sp", "tp"),
            P("sp", "tp"),
        ),
        out_specs=(
            P("sp", "tp"),
            P("sp", "tp"),
            P("sp", "tp"),
            P("sp", None, "tp"),
            P("sp", None, "tp"),
            P("sp", "tp", None),
        ),
        check_vma=False,
    )
```
